32 devices in a mesh: sp: 8 (over z, x), dp: 4 (over y, core).
Axes of the slice: x: 2, y: 2, z: 4, core: 2. Of those that a mesh axis runs over, the one named last changes fastest.
Arguments:
- tokens: bfloat16 [4, 4096, 4096], P('dp', 'sp'), may hold values from -6 to 6
- documents: int32 [4, 4096], P('dp', 'sp'), may hold values from 0 to 7, never falling along the last dimension, each value on 1 to 1024 neighbouring positions
- value_weight: bfloat16 [4096, 2048], P(('sp', 'dp')), may hold values from -0.09375 to 0.09375
- gate_weight: bfloat16 [4096, 2048], P(('sp', 'dp')), may hold values from -0.09375 to 0.09375
- conv_weight: bfloat16 [31, 2048], replicated, may hold values from -1 to 1
- norm_gain: float32 [2048], replicated, may hold values from 0.1 to 1.9
- norm_bias: float32 [2048], replicated, may hold values from -2 to 2
Outputs:
- activated: bfloat16 [4, 4096, 2048], P('dp', 'sp')
The draws below stay inside these ranges and needn't reach their ends.
Inputs may be any that keep to these rules, and one draw needn't show every extreme that they name: `documents`: document numbers never fall along a sequence, run from 0 to 7, and each document covers 1 to 1024 positions.
All inputs are finite; a program needn't handle non-finite values.
Results may differ from the reference program's by a relative error of at most 0.0064.
Values may be sent and summed in bfloat16 or wider, within the bound.
A program may use at most 192 MiB of HBM per device.

```python
import math
import jax
import jax.numpy as jnp
import numpy as np
from jax import lax

D = 4096
DB = 2048
KERNEL = 31
DOCS = 8
LENGTH = 4096
BATCH = 4


def levels(key, extent, pieces, smallest, high):
    def one(position, blocks):
        heights = jax.random.uniform(jax.random.fold_in(jax.random.fold_in(key, 6), position), (blocks,), jnp.float32, smallest / len(pieces), high / len(pieces))
        return jnp.repeat(jnp.exp(heights), extent[position] // blocks).reshape((-1,) + (1,) * (len(extent) - position - 1))

    factor_of = one(*pieces[0])
    for cut in pieces[1:]:
        factor_of = factor_of * one(*cut)
    return factor_of


def length_profile(amount, total, most, lean):
    portions = [(1 << 20) // math.isqrt(standing ** lean) + 1 for standing in range(2, amount + 1)]
    surplus, given = total - most - (amount - 1), [1] * (amount - 1)
    while surplus > 0:
        candidates = [i for i in range(amount - 1) if given[i] < most]
        pool, budget = sum([portions[i] for i in candidates]), surplus
        for i in candidates:
            extra = min(most - given[i], max(1, budget * portions[i] // pool), surplus)
            given[i] = given[i] + extra
            surplus = surplus - extra
    return np.array([most] + given)


def uneven(stream_key, number_of, total, reach, lean):
    if number_of == 2:
        one = jax.random.randint(stream_key, (), max(1, total - reach), min(reach, total - 1) + 1)
        return jnp.stack([one, total - one])
    tallies = jnp.asarray(length_profile(number_of, total, reach, lean), jnp.int32)
    twos = (number_of - 1) // 2
    donor, sink = tallies[1:1 + 2 * twos:2], tallies[2:2 + 2 * twos:2]
    slack = jnp.minimum(donor - 1, reach - sink)
    shifted = jax.random.randint(jax.random.fold_in(stream_key, 1), (twos,), 0, 1 << 20) % (slack + 1)
    tallies = tallies.at[1:1 + 2 * twos:2].set(donor - shifted).at[2:2 + 2 * twos:2].set(sink + shifted)
    return tallies[jax.random.permutation(jax.random.fold_in(stream_key, 2), number_of)]


def bell_draw(stream_key, dims, scale, bound, cuts=(), dtype=jnp.bfloat16):
    factor_of = levels(stream_key, dims, cuts, -0.22, 0.18) if cuts else 1.0
    entries = jax.random.normal(stream_key, dims, jnp.float32) * scale * factor_of
    return jnp.minimum(jnp.maximum(entries, -bound), bound).astype(dtype)


def setup_inputs(seed: int = 0) -> dict:
    streams_of = jax.random.split(jax.random.key(seed), 8)
    tokens = bell_draw(streams_of[0], (BATCH, LENGTH, D), 1.0, 6.0, ((0, 4), (1, 8)))
    documents = jax.vmap(lambda own: jnp.searchsorted(jnp.cumsum(uneven(own, DOCS, LENGTH, LENGTH // 4, 1)), jnp.arange(LENGTH), side="right"))(jax.random.split(streams_of[1], BATCH)).reshape((BATCH, LENGTH)).astype(jnp.int32)
    value_weight = bell_draw(streams_of[2], (D, DB), D ** -0.5, 0.09375, ((0, 32),))
    gate_weight = bell_draw(streams_of[3], (D, DB), D ** -0.5, 0.09375, ((0, 32),))
    conv_weight = bell_draw(streams_of[4], (KERNEL, DB), KERNEL ** -0.5, 1.0)
    norm_gain = jnp.clip(1.0 + 0.18 * jax.random.normal(streams_of[5], (DB,), jnp.float32), 0.1, 1.9)
    norm_bias = bell_draw(streams_of[6], (DB,), 0.5, 2.0, (), jnp.float32)
    return dict(tokens=tokens, documents=documents, value_weight=value_weight, gate_weight=gate_weight, conv_weight=conv_weight, norm_gain=norm_gain, norm_bias=norm_bias)


def convolve(padded, padded_docs, taps, count):
    lead = taps.shape[0] - 1
    here = padded_docs[:, lead:lead + count]
    total = jnp.zeros((padded.shape[0], count, padded.shape[2]), jnp.float32)
    for lag in range(taps.shape[0]):
        begin = lead - lag
        moved = padded[:, begin:begin + count].astype(jnp.float32)
        keep = (padded_docs[:, begin:begin + count] == here)[:, :, None]
        total = total + jnp.where(keep, moved, 0.0) * taps[lag].astype(jnp.float32)
    return total

def finish(mixed, norm_gain, norm_bias):
    wide = mixed.astype(jnp.float32)
    center = wide - lax.optimization_barrier(jnp.mean(wide, axis=-1, keepdims=True))
    spread = lax.optimization_barrier(jnp.mean(center * center, axis=-1, keepdims=True))
    normed = center * lax.rsqrt(spread + 1e-06) * norm_gain + norm_bias
    return jax.nn.silu(normed).astype(jnp.bfloat16)

def reference(tokens, documents, value_weight, gate_weight, conv_weight, norm_gain, norm_bias):
    lead = KERNEL - 1

    def one_row(pair):
        rows, row_docs = pair
        value = jnp.dot(rows, value_weight, preferred_element_type=jnp.float32).astype(jnp.bfloat16)
        gate = jnp.dot(rows, gate_weight, preferred_element_type=jnp.float32).astype(jnp.bfloat16)
        value, gate = lax.optimization_barrier((value, gate))
        glu = (value.astype(jnp.float32) * jax.nn.sigmoid(gate.astype(jnp.float32))).astype(jnp.bfloat16)
        glu = lax.optimization_barrier(glu)
        padded = jnp.pad(glu[None], ((0, 0), (lead, 0), (0, 0)))
        padded_docs = jnp.pad(row_docs[None], ((0, 0), (lead, 0)), constant_values=-1)
        mixed = convolve(padded, padded_docs, conv_weight, rows.shape[0]).astype(jnp.bfloat16)
        mixed = lax.optimization_barrier(mixed)
        return finish(mixed, norm_gain, norm_bias)[0]
    return lax.map(one_row, (tokens, documents))
```

```python
import functools

import jax
import jax.numpy as jnp
from jax import lax
from jax.experimental import pallas as pl
from jax.experimental.pallas import tpu as pltpu
from jax.sharding import PartitionSpec as P

KERNEL = 31
BLOCKS = 4
HALO = 32
MESH = pl.DeviceIdType.MESH


def gather_kernel(
    side, tall, tok_hbm, own_hbm, glu_ref, weights, tok, send, recv, cross, begin, halo
):
    sp, dp = lax.axis_index("sp"), lax.axis_index("dp")
    sp_size = lax.axis_size("sp")
    core, y = lax.rem(dp, 2), lax.div(dp, 2)
    z, x = lax.div(sp, side), lax.rem(sp, side)
    flip = core == 1
    u, v = jnp.where(flip, y, x), jnp.where(flip, x, y)
    half = own_hbm.shape[2]
    depth = 2 * half
    count = tok_hbm.shape[0]
    sub = tall // 2
    columns = weights.shape[3] // sub
    wide = columns // 2
    other = {"sp": sp, "dp": y * 2 + (1 - core)}

    def device(dz, du, dv):
        dx, dy = jnp.where(flip, dv, du), jnp.where(flip, du, dv)
        return {"sp": dz * side + dx, "dp": dy * 2 + core}

    def number(pz, pu, pv):
        px, py = jnp.where(flip, pv, pu), jnp.where(flip, pu, pv)
        return (pz * side + px) * side + py

    def piece(plane, block, q):
        return weights.at[plane, block, pl.ds(pl.multiple_of(q * depth, depth), depth), :]

    def link(kind, block, q, target):
        return pltpu.make_async_remote_copy(
            src_ref=piece(core, block, q),
            dst_ref=piece(core, block, q),
            send_sem=send.at[kind, block, q],
            recv_sem=recv.at[block, q],
            device_id=target,
            device_id_type=MESH,
        )

    def hand_over(plane, block, q):
        return pltpu.make_async_remote_copy(
            src_ref=piece(plane, block, q),
            dst_ref=piece(plane, block, q),
            send_sem=send.at[6, block, q],
            recv_sem=cross.at[block, q],
            device_id=other,
            device_id_type=MESH,
        )

    def routes(block, pz, pu, pv, act):
        q = number(pz, pu, pv)
        tall_first = block == 1
        home_u, home_v, home_z = u == pu, v == pv, z == pz
        along_z = home_v & (home_u | jnp.logical_not(tall_first))
        along_u = home_v & (home_z | tall_first)
        ways = (
            (along_z & (z >= pz) & (z + 1 < tall), (z + 1, u, v)),
            (along_z & (z <= pz) & (z > 0), (z - 1, u, v)),
            (along_u & (u >= pu) & (u + 1 < side), (z, u + 1, v)),
            (along_u & (u <= pu) & (u > 0), (z, u - 1, v)),
            ((v >= pv) & (v + 1 < side), (z, u, v + 1)),
            ((v <= pv) & (v > 0), (z, u, v - 1)),
        )
        for kind, (taken, target) in enumerate(ways):

            @pl.when(taken)
            def _(kind=kind, target=target):
                act(link(kind, block, q, device(*target)))

        @pl.when(jnp.logical_not(home_u & home_v & home_z))
        def _():
            act(hand_over(core, block, q))

    def pass_on(block, pz, pu, pv):
        routes(block, pz, pu, pv, lambda copy: copy.start())

    def arrived(block, pz, pu, pv):
        link(0, block, number(pz, pu, pv), other).wait_recv()
        pass_on(block, pz, pu, pv)

    low = jnp.minimum(z, tall - 1 - z)

    def near(k):
        step = jnp.where(lax.rem(k, 2) == 1, low - lax.div(k + 1, 2), low + lax.div(k, 2))
        at = jnp.where(k <= 2 * low, step, k)
        return jnp.where(z == low, at, tall - 1 - at)

    barrier = pltpu.get_barrier_semaphore()
    greeted = jnp.int32(1)
    pl.semaphore_signal(barrier, inc=1, device_id=other, device_id_type=MESH)
    for there, target in (
        (z + 1 < tall, device(z + 1, u, v)),
        (z > 0, device(z - 1, u, v)),
        (u + 1 < side, device(z, u + 1, v)),
        (u > 0, device(z, u - 1, v)),
        (v + 1 < side, device(z, u, v + 1)),
        (v > 0, device(z, u, v - 1)),
        (sp + 1 < sp_size, {"sp": sp + 1, "dp": dp}),
        (sp > 0, {"sp": sp - 1, "dp": dp}),
    ):
        greeted = greeted + there.astype(jnp.int32)

        @pl.when(there)
        def _(target=target):
            pl.semaphore_signal(barrier, inc=1, device_id=target, device_id_type=MESH)

    pl.semaphore_wait(barrier, greeted)

    here = (z * side + x) * side + y
    own_rows = weights.at[
        :, :, pl.ds(pl.multiple_of(here * depth + core * half, half), half), :
    ]
    to_other = pltpu.make_async_remote_copy(
        src_ref=own_hbm,
        dst_ref=own_rows,
        send_sem=begin.at[0],
        recv_sem=begin.at[1],
        device_id=other,
        device_id_type=MESH,
    )
    to_other.start()
    keep = pltpu.make_async_copy(own_hbm, own_rows, begin.at[2])
    keep.start()
    load = pltpu.make_async_copy(tok_hbm, tok.at[pl.ds(HALO, count), :], begin.at[3])
    load.start()
    tail = pltpu.make_async_remote_copy(
        src_ref=tok_hbm.at[pl.ds(count - HALO, HALO), :],
        dst_ref=tok.at[pl.ds(0, HALO), :],
        send_sem=halo.at[0],
        recv_sem=halo.at[1],
        device_id={"sp": lax.rem(sp + 1, sp_size), "dp": dp},
        device_id_type=MESH,
    )

    @pl.when(sp + 1 < sp_size)
    def _():
        tail.start()

    @pl.when(sp == 0)
    def _():
        tok[pl.ds(0, HALO), :] = jnp.zeros((HALO, tok.shape[1]), tok.dtype)

    keep.wait()
    to_other.wait_recv()
    pass_on(0, z, u, v)
    load.wait()

    @pl.when(sp > 0)
    def _():
        tail.wait_recv()

    def tick(at, carry):
        block, k = lax.div(at, tall), lax.rem(at, tall)

        @pl.when((block < BLOCKS) & (k > 0))
        def _():
            arrived(block, near(k), u, v)

        @pl.when((block + 1 < BLOCKS) & (k == 0))
        def _():
            pass_on(block + 1, z, u, v)

        second = jnp.maximum(at - 1, 0)
        block2, k2 = lax.div(second, tall), lax.rem(second, tall)

        @pl.when((at >= 1) & (block2 < BLOCKS))
        def _():
            @pl.loop(1, side)
            def _(du):
                arrived(block2, near(k2), lax.rem(u + du, side), v)

        third = jnp.maximum(at - 2, 0)
        block3, k3 = lax.div(third, tall), lax.rem(third, tall)

        @pl.when((at >= 2) & (block3 < BLOCKS))
        def _():
            @pl.loop(0, side)
            def _(du):
                @pl.loop(1, side)
                def _(dv):
                    arrived(block3, near(k3), lax.rem(u + du, side), lax.rem(v + dv, side))

        late = jnp.maximum(at - tall - 2, 0)
        block4, k4 = lax.div(late, tall), lax.rem(late, tall)

        @pl.when((at >= tall + 2) & (k4 == 0))
        def _():
            @pl.loop(0, tall * side * side)
            def _(q):
                @pl.when(q != here)
                def _():
                    hand_over(1 - core, block4, q).wait_recv()

        @pl.when(at >= tall + 2)
        def _():
            plane, part = lax.div(k4, sub), lax.rem(k4, sub)
            held = weights[
                plane, block4, :, pl.ds(pl.multiple_of(part * columns, columns), columns)
            ]
            both = jnp.dot(tok[...], held, preferred_element_type=jnp.float32)
            value = both[:, :wide].astype(jnp.bfloat16).astype(jnp.float32)
            gate = both[:, wide:].astype(jnp.bfloat16).astype(jnp.float32)
            first = ((plane * BLOCKS + block4) * sub + part) * wide
            glu_ref[:, pl.ds(pl.multiple_of(first, wide), wide)] = (
                value * jax.nn.sigmoid(gate)
            ).astype(jnp.bfloat16)

        return carry

    lax.fori_loop(0, BLOCKS * tall + tall + 2, tick, 0)

    @pl.loop(0, BLOCKS)
    def _(block):
        @pl.loop(0, tall)
        def _(pz):
            @pl.loop(0, side)
            def _(pu):
                @pl.loop(0, side)
                def _(pv):
                    routes(block, pz, pu, pv, lambda copy: copy.wait_send())

    to_other.wait_send()

    @pl.when(sp + 1 < sp_size)
    def _():
        tail.wait_send()


def gated_product(rows, value_weight, gate_weight):
    side = lax.axis_size("dp") // 2
    tall = lax.axis_size("sp") // side
    count, width = rows.shape
    depth, channels = value_weight.shape
    wide = channels // (BLOCKS * tall)
    cut = (depth, 2, BLOCKS, tall // 2, 1, wide)
    own = jnp.concatenate([value_weight.reshape(cut), gate_weight.reshape(cut)], axis=4)
    own = own.transpose(1, 2, 0, 3, 4, 5).reshape(2, BLOCKS, depth, channels // BLOCKS)
    pieces = tall * side * side
    return pl.pallas_call(
        functools.partial(gather_kernel, side, tall),
        out_shape=jax.ShapeDtypeStruct((HALO + count, channels), jnp.bfloat16),
        in_specs=[pl.BlockSpec(memory_space=pl.ANY)] * 2,
        out_specs=pl.BlockSpec(memory_space=pltpu.VMEM),
        scratch_shapes=[
            pltpu.VMEM((2, BLOCKS, width, channels // BLOCKS), jnp.bfloat16),
            pltpu.VMEM((HALO + count, width), jnp.bfloat16),
            pltpu.SemaphoreType.DMA((7, BLOCKS, pieces)),
            pltpu.SemaphoreType.DMA((BLOCKS, pieces)),
            pltpu.SemaphoreType.DMA((BLOCKS, pieces)),
            pltpu.SemaphoreType.DMA((4,)),
            pltpu.SemaphoreType.DMA((2,)),
        ],
        compiler_params=pltpu.CompilerParams(
            collective_id=0, has_side_effects=True, vmem_limit_bytes=56 * 1024 * 1024
        ),
    )(rows, own)


def passed_along(block, axis, distance):
    devices = range(lax.axis_size(axis))
    route = [(i - distance, i) for i in devices if i - distance in devices]
    return lax.ppermute(block, axis, route)


def mix_kernel(glu_ref, reach_ref, taps_ref, gain_ref, bias_ref, out_ref, mixed):
    rows, channels = out_ref.shape
    top = pl.multiple_of(pl.program_id(0) * rows, rows)
    reach = reach_ref[...]

    @pl.loop(0, channels // 128)
    def _(lane):
        lanes = pl.ds(pl.multiple_of(lane * 128, 128), 128)
        window = glu_ref[pl.ds(top, rows + HALO), lanes].astype(jnp.float32)
        total = jnp.zeros((rows, 128), jnp.float32)
        for shift in range(8):
            held = window if shift == 0 else window[shift : shift + rows + HALO - 8]
            for offset in range(shift, HALO + 1, 8):
                lag = HALO - offset
                if lag < KERNEL:
                    moved = held[offset - shift : offset - shift + rows]
                    moved = jnp.where(reach >= lag, moved, 0.0)
                    total = total + moved * taps_ref[lag : lag + 1, lanes]
        mixed[:, lanes] = total.astype(jnp.bfloat16).astype(jnp.float32)

    wide = mixed[...]
    center = wide - jnp.mean(wide, axis=-1, keepdims=True)
    spread = jnp.mean(center * center, axis=-1, keepdims=True)
    normed = center * lax.rsqrt(spread + 1e-06) * gain_ref[...] + bias_ref[...]
    out_ref[...] = (normed * jax.nn.sigmoid(normed)).astype(jnp.bfloat16)


def mix_and_finish(glu, reach, taps, norm_gain, norm_bias):
    channels = glu.shape[1]
    count = reach.shape[0]
    rows = 64
    return pl.pallas_call(
        mix_kernel,
        grid=(count // rows,),
        out_shape=jax.ShapeDtypeStruct((count, channels), jnp.bfloat16),
        in_specs=[
            pl.BlockSpec(glu.shape, lambda i: (0, 0)),
            pl.BlockSpec((rows, 128), lambda i: (i, 0)),
            pl.BlockSpec(taps.shape, lambda i: (0, 0)),
            pl.BlockSpec((1, channels), lambda i: (0, 0)),
            pl.BlockSpec((1, channels), lambda i: (0, 0)),
        ],
        out_specs=pl.BlockSpec((rows, channels), lambda i: (i, 0)),
        scratch_shapes=[pltpu.VMEM((rows, channels), jnp.float32)],
    )(glu, reach, taps, norm_gain[None], norm_bias[None])


def per_device(tokens, documents, value_weight, gate_weight, conv_weight, norm_gain, norm_bias):
    batch, count, width = tokens.shape
    channels = value_weight.shape[1]
    lead = KERNEL - 1
    rows = tokens.reshape(batch * count, width)
    docs = documents.reshape(count)
    before_docs = passed_along(docs[count - lead :], "sp", 1)
    before_docs = jnp.where(lax.axis_index("sp") == 0, -1, before_docs)
    docs_wide = jnp.concatenate([before_docs, docs])
    reach = jnp.zeros((count,), jnp.int32)
    for lag in range(1, KERNEL):
        reach = reach + (docs_wide[lead - lag : lead - lag + count] == docs).astype(jnp.int32)
    reach = jnp.broadcast_to(reach[:, None], (count, 128))
    glu = gated_product(rows, value_weight, gate_weight)
    taps = jnp.pad(conv_weight.astype(jnp.float32), ((0, 1), (0, 0)))
    out = mix_and_finish(glu, reach, taps, norm_gain, norm_bias)
    return out.reshape(batch, count, channels)


def solution(mesh):
    return jax.shard_map(
        per_device,
        mesh=mesh,
        in_specs=(
            P("dp", "sp", None),
            P("dp", "sp"),
            P(("sp", "dp"), None),
            P(("sp", "dp"), None),
            P(),
            P(),
            P(),
        ),
        out_specs=P("dp", "sp", None),
        check_vma=False,
    )
```
